32 devices in a mesh: fs: 16 (over z, y, x), tp: 2 (over core).
Axes of the slice: x: 2, y: 2, z: 4, core: 2. Of those that a mesh axis runs over, the one named last changes fastest.
Arguments:
- fwd_tokens: bfloat16 [2048, 2048], P('fs'), may hold values from -6 to 6
- back_tokens: bfloat16 [2048, 2048], P('fs'), may hold values from -6 to 6
- out_grad: bfloat16 [2048, 2048], P('fs'), may hold values from -6 to 6
- norm_gain: float32 [2048], replicated, may hold values from 0.1 to 1.9
- gate_weight: bfloat16 [2048, 2816], P('fs', 'tp'), may hold values from -0.125 to 0.125
- up_weight: bfloat16 [2048, 2816], P('fs', 'tp'), may hold values from -0.125 to 0.125
- down_weight: bfloat16 [2048, 2816], P('fs', 'tp'), may hold values from -0.109375 to 0.109375
- gate_grad_sum: float32 [2048, 2816], P('fs', 'tp'), may hold values from -96 to 96
Outputs:
- fwd_out: bfloat16 [2048, 2048], P('fs')
- back_grad: bfloat16 [2048, 2048], P('fs')
- gate_grad_out: float32 [2048, 2816], P('fs', 'tp')
The draws below stay inside these ranges and needn't reach their ends.
All inputs are finite; a program needn't handle non-finite values.
Results may differ from the reference program's by a relative error of at most 0.014.
Values may be sent and summed in bfloat16 or wider, within the bound.
A program may use at most 64 MiB of HBM per device.

```python
import jax
import jax.numpy as jnp
from jax import lax

D = 2048
FF = 2816
TOKENS = 2048
N_TP = 2


def spiked(entries, own_key, source, target, parts, factor):
    def block_of(dim):
        return (jnp.arange(entries.shape[dim]) // (entries.shape[dim] // parts)).reshape((-1,) + (1,) * (entries.ndim - 1 - dim))

    near = jax.random.permutation(own_key, parts)[block_of(target)]
    far = (block_of(target) + parts // 2) % parts
    return jnp.where((block_of(source) == near) | (block_of(source) == far), factor * entries, entries)


def level_of(key, shape, pieces, smallest, high):
    def one(position, blocks):
        draws = jax.random.uniform(jax.random.fold_in(jax.random.fold_in(key, 6), position), (blocks,), jnp.float32, smallest / len(pieces), high / len(pieces))
        return jnp.repeat(jnp.exp(draws), shape[position] // blocks).reshape((-1,) + (1,) * (len(shape) - position - 1))

    gain = one(*pieces[0])
    for cut in pieces[1:]:
        gain = gain * one(*cut)
    return gain


def scatter_about(own_key, shape, spread, bound, split=(), kind=jnp.bfloat16):
    entries = spread * jax.random.normal(own_key, shape, jnp.float32)
    if split:
        entries = entries * level_of(own_key, shape, split, -0.22, 0.18)
    return jnp.clip(entries, -bound, bound).astype(kind)


def noise_with(key, shape, width, most, split, heavy, kind=jnp.bfloat16):
    drawn = width * jax.random.normal(key, shape, jnp.float32)
    if split:
        drawn = drawn * level_of(key, shape, split, -0.22, 0.18)
    return jnp.clip(spiked(drawn, jax.random.fold_in(key, 3), *heavy), -most, most).astype(kind)


def setup_inputs(seed: int = 0) -> dict:
    streams_of = jax.random.split(jax.random.key(seed), 9)
    return {
        "fwd_tokens": scatter_about(streams_of[0], (TOKENS, D), 1.0, 6.0, ((0, 16),)),
        "back_tokens": noise_with(streams_of[1], (TOKENS, D), 1.0, 6.0, ((0, 16),), (0, 1, 16, 2.0)),
        "out_grad": noise_with(streams_of[2], (TOKENS, D), 1.0, 6.0, ((0, 16),), (0, 1, 16, 2.0)),
        "norm_gain": jnp.clip(1.0 + 0.18 * jax.random.normal(streams_of[3], (D,), jnp.float32), 0.1, 1.9),
        "gate_weight": scatter_about(streams_of[4], (D, FF), D ** -0.5, 0.125, ((0, 16), (1, 2))),
        "up_weight": scatter_about(streams_of[5], (D, FF), D ** -0.5, 0.125, ((0, 16), (1, 2))),
        "down_weight": scatter_about(streams_of[6], (D, FF), FF ** -0.5, 0.109375, ((0, 16), (1, 2))),
        "gate_grad_sum": scatter_about(streams_of[7], (D, FF), 16.0, 96.0, ((0, 16), (1, 2)), jnp.float32),
    }


norm_eps = 0.25

def normalize(tokens, norm_gain):
    values = tokens.astype(jnp.float32)
    factor = lax.rsqrt(lax.optimization_barrier(jnp.mean(values * values, axis=-1, keepdims=True)) + norm_eps)
    return (values, factor, (values * factor * norm_gain).astype(jnp.bfloat16))

def rounded(block_part):
    return lax.optimization_barrier(block_part.astype(jnp.bfloat16)).astype(jnp.float32)

def reference(fwd_tokens, back_tokens, out_grad, norm_gain, gate_weight, up_weight, down_weight, gate_grad_sum):
    col_width = FF // N_TP
    fwd_normed = normalize(fwd_tokens, norm_gain)[2]
    gate_pre = jnp.dot(fwd_normed, gate_weight, preferred_element_type=jnp.float32)
    up_pre = jnp.dot(fwd_normed, up_weight, preferred_element_type=jnp.float32)
    hidden = (gate_pre * jax.nn.sigmoid(gate_pre) * up_pre).astype(jnp.bfloat16)
    summed = jnp.zeros((TOKENS, D), jnp.float32)
    for tp_block in range(N_TP):
        lower = tp_block * col_width
        upper = lower + col_width
        block_part = jnp.dot(hidden[:, lower:upper], down_weight[:, lower:upper].T, preferred_element_type=jnp.float32)
        summed = summed + rounded(block_part)
    fwd_out = (0.5 * summed).astype(jnp.bfloat16)
    values, factor, back_normed = normalize(back_tokens, norm_gain)
    gate_pre = jnp.dot(back_normed, gate_weight, preferred_element_type=jnp.float32)
    up_pre = jnp.dot(back_normed, up_weight, preferred_element_type=jnp.float32)
    sigmoid_gate = jax.nn.sigmoid(gate_pre)
    back_hidden = 0.5 * jnp.dot(out_grad, down_weight, preferred_element_type=jnp.float32)
    gate_diff = (back_hidden * up_pre * sigmoid_gate * (1.0 + gate_pre * (1.0 - sigmoid_gate))).astype(jnp.bfloat16)
    up_diff = (back_hidden * gate_pre * sigmoid_gate).astype(jnp.bfloat16)
    normed_diff = jnp.zeros((TOKENS, D), jnp.float32)
    for tp_block in range(N_TP):
        lower = tp_block * col_width
        upper = lower + col_width
        block_part = jnp.dot(gate_diff[:, lower:upper], gate_weight[:, lower:upper].T, preferred_element_type=jnp.float32)
        block_part = block_part + jnp.dot(up_diff[:, lower:upper], up_weight[:, lower:upper].T, preferred_element_type=jnp.float32)
        normed_diff = normed_diff + rounded(block_part)
    scaled = normed_diff * norm_gain
    cubed = factor * factor * factor
    back_grad = (factor * scaled - values * cubed * lax.optimization_barrier(jnp.mean(scaled * values, axis=-1, keepdims=True))).astype(jnp.bfloat16)
    gate_grad_out = gate_grad_sum + jnp.dot(back_normed.T, gate_diff, preferred_element_type=jnp.float32)
    return (fwd_out, back_grad, gate_grad_out)
```

```python
import functools

import jax
import jax.numpy as jnp
from jax import lax
from jax.experimental import pallas as pl
from jax.experimental.pallas import tpu as pltpu
from jax.sharding import PartitionSpec as P

norm_eps = 0.25


def normalize(tokens, norm_gain):
    values = tokens.astype(jnp.float32)
    factor = lax.rsqrt(jnp.mean(values * values, axis=-1, keepdims=True) + norm_eps)
    return (values, factor, (values * factor * norm_gain).astype(jnp.bfloat16))


def shards(
    fwd_tokens, back_tokens, out_grad, norm_gain, gate_weight, up_weight, down_weight, gate_grad_sum
):
    fwd_normed = normalize(fwd_tokens, norm_gain)[2]
    columns = fwd_normed
    gate_pre = jnp.dot(
        columns,
        lax.all_gather(gate_weight, "fs", axis=0, tiled=True),
        preferred_element_type=jnp.float32,
    )
    up_pre = jnp.dot(
        columns,
        lax.all_gather(up_weight, "fs", axis=0, tiled=True),
        preferred_element_type=jnp.float32,
    )
    hidden = (gate_pre * jax.nn.sigmoid(gate_pre) * up_pre).astype(jnp.bfloat16)
    partial_value = jnp.dot(
        hidden,
        lax.all_gather(down_weight, "fs", axis=0, tiled=True).T,
        preferred_element_type=jnp.float32,
    )
    summed = lax.psum(partial_value.astype(jnp.bfloat16), "tp").astype(jnp.float32)
    fwd_out = (0.5 * summed).astype(jnp.bfloat16)
    gate_whole = lax.all_gather(gate_weight, "fs", axis=0, tiled=True)
    up_whole = lax.all_gather(up_weight, "fs", axis=0, tiled=True)
    down_whole = lax.all_gather(down_weight, "fs", axis=0, tiled=True)
    values, factor, back_normed = normalize(back_tokens, norm_gain)
    gate_pre = jnp.dot(back_normed, gate_whole, preferred_element_type=jnp.float32)
    up_pre = jnp.dot(back_normed, up_whole, preferred_element_type=jnp.float32)
    sigmoid_gate = jax.nn.sigmoid(gate_pre)
    back_hidden = 0.5 * jnp.dot(out_grad, down_whole, preferred_element_type=jnp.float32)
    gate_diff = (
        back_hidden * up_pre * sigmoid_gate * (1.0 + gate_pre * (1.0 - sigmoid_gate))
    ).astype(jnp.bfloat16)
    up_diff = (back_hidden * gate_pre * sigmoid_gate).astype(jnp.bfloat16)
    columns = back_normed
    gate_grad_out = gate_grad_sum + lax.psum_scatter(
        jnp.dot(columns.T, gate_diff, preferred_element_type=jnp.float32),
        "fs",
        scatter_dimension=0,
        tiled=True,
    )
    partial_diff = jnp.dot(gate_diff, gate_whole.T, preferred_element_type=jnp.float32)
    partial_diff = partial_diff + jnp.dot(up_diff, up_whole.T, preferred_element_type=jnp.float32)
    normed_diff = lax.psum(partial_diff.astype(jnp.bfloat16), "tp").astype(jnp.float32)
    scaled = normed_diff * norm_gain
    cubed = factor * factor * factor
    back_grad = (
        factor * scaled - values * cubed * jnp.mean(scaled * values, axis=-1, keepdims=True)
    ).astype(jnp.bfloat16)
    back_grad, gate_grad_out = (back_grad, gate_grad_out)
    return (fwd_out, back_grad, gate_grad_out)


MESH = pl.DeviceIdType.MESH


def wide_dot(a, b):
    return lax.dot_general(a, b, (((1,), (1,)), ((), ())), preferred_element_type=jnp.float32)


def layer_kernel(
    planes, plane, fwd_ref, back_ref, grad_ref, tokens_ref, gain_ref, gate_ref, up_ref, down_ref, sum_ref,
    fwd_out, back_out, sum_out,
    toks, weights, fwd_gate, fwd_up, back_gate, back_up, hidden, gate_diff, up_diff,
    part, crossed, joined, gathered, grad_send, grad_recv, grad_cols,
    stage_sem, weight_sem, up_sem, down_sem, tok_send, tok_recv, relay_send, relay_recv,
    grad_send_sem, grad_recv_sem, cross_sem, join_send, join_recv, last_sem,
):
    n_fs = planes * plane
    fs, core = lax.axis_index("fs"), lax.axis_index("tp")
    level, place = fs // plane, fs % plane
    sibling = (fs, 1 - core)
    rows = weights.shape[1]
    depth = gate_ref.shape[1]
    half = fwd_ref.shape[0] // 2
    slab = half * plane
    width = fwd_ref.shape[1]

    barrier = pltpu.get_barrier_semaphore()
    for step in range(1, n_fs):
        pl.semaphore_signal(barrier, inc=1, device_id=((fs + step) % n_fs, core), device_id_type=MESH)
    pl.semaphore_signal(barrier, inc=1, device_id=sibling, device_id_type=MESH)
    pl.semaphore_wait(barrier, n_fs)

    def remote(src, dst, send, recv, device):
        return pltpu.make_async_remote_copy(
            src_ref=src, dst_ref=dst, send_sem=send, recv_sem=recv, device_id=device, device_id_type=MESH
        )

    own = (gate_ref, up_ref, down_ref)

    def own_block(w, q):
        return own[w].at[pl.ds(pl.multiple_of(q * rows, rows), rows), :]

    def block(w, src):
        return weights.at[w, :, pl.ds(pl.multiple_of(src * depth, depth), depth)]

    def staged(w, step):
        q = (place + step) % plane
        return remote(own_block(w, q), block(w, fs), stage_sem.at[w, step], weight_sem.at[w, fs], (level * plane + q, core))

    def arrived(w, src):
        remote(block(w, src), block(w, src), stage_sem.at[w, 0], weight_sem.at[w, src], sibling).wait_recv()

    def hop(w, src, source, step):
        sem = up_sem if step > 0 else down_sem
        return remote(source, block(w, src), sem.at[w, src], weight_sem.at[w, src], ((fs + step * plane + n_fs) % n_fs, core))

    can = {1: level < planes - 1, -1: level > 0}

    def send_on(w, src, source, step):
        @pl.when(can[step])
        def _():
            hop(w, src, source, step).start()

    token_refs = (back_ref, fwd_ref, grad_ref)

    def tok_block(a, h, q):
        return toks.at[a, h, pl.ds(pl.multiple_of(q * half, half), half), :]

    def tok_copy(a, step):
        q = (place + step) % plane
        return remote(
            token_refs[a].at[pl.ds(pl.multiple_of(core * half, half), half), :],
            tok_block(a, core, place), tok_send.at[a, step], tok_recv.at[a, place], (level * plane + q, core),
        )

    def tok_arrived(a, q):
        remote(tok_block(a, core, q), tok_block(a, core, q), tok_send.at[a, 0], tok_recv.at[a, q], sibling).wait_recv()

    def relay(a, q):
        return remote(tok_block(a, core, q), tok_block(a, core, q), relay_send.at[a, q], relay_recv.at[a, q], sibling)

    def relayed(a, q):
        remote(tok_block(a, 1 - core, q), tok_block(a, 1 - core, q), relay_send.at[a, q], relay_recv.at[a, q], sibling).wait_recv()

    for w in range(3):
        for step in range(1, plane):
            staged(w, step).start()
        for step in (1, -1):
            send_on(w, fs, own_block(w, place), step)
    for a in range(3):
        for step in range(1, plane):
            tok_copy(a, step).start()
    for w in range(3):
        weights[w, :, pl.ds(pl.multiple_of(fs * depth, depth), depth)] = own[w][pl.ds(pl.multiple_of(place * rows, rows), rows), :]
    for a in range(3):
        for h in range(2):
            toks[a, h, pl.ds(pl.multiple_of(place * half, half), half), :] = token_refs[a][pl.ds(h * half, half), :]

    def group(w, d):
        if d == 0:
            for step in range(1, plane):
                src = level * plane + (place + step) % plane
                arrived(w, src)
                for way in (1, -1):
                    send_on(w, src, block(w, src), way)
            return
        for way in (1, -1):
            other = level - way * d

            @pl.when(jnp.logical_and(other >= 0, other < planes))
            def _():
                @pl.loop(0, plane)
                def _(q):
                    src = other * plane + q
                    arrived(w, src)
                    send_on(w, src, block(w, src), way)

    def relays(a):
        for step in range(1, plane):
            q = (place + step) % plane
            tok_arrived(a, q)
            relay(a, q).start()

    def relays_in(a):
        for step in range(1, plane):
            relayed(a, (place + step) % plane)

    def project(a, w, out):
        @pl.loop(0, 2)
        def _(h):
            out[h] = wide_dot(toks[a, h], weights[w])

    for wave in range(planes):
        for w in range(3):
            d = wave - w
            if 0 <= d < planes:
                group(w, d)
    relays(0)
    relays(1)
    relays_in(0)
    project(0, 0, back_gate)
    relays_in(1)
    project(1, 0, fwd_gate)
    relays(2)
    for w in range(1, 3):
        if 0 <= planes - w < planes:
            group(w, planes - w)
    relays_in(2)
    project(0, 1, back_up)
    project(1, 1, fwd_up)

    piece = 64

    @pl.loop(0, 2)
    def _(h):
        @pl.loop(0, slab // piece)
        def _(r):
            at = pl.ds(pl.multiple_of(r * piece, piece), piece)
            gate = fwd_gate[h, at, :]
            hidden[h, at, :] = (gate * jax.nn.sigmoid(gate) * fwd_up[h, at, :]).astype(jnp.bfloat16)
            gate = back_gate[h, at, :]
            s = jax.nn.sigmoid(gate)
            back_gate[h, at, :] = gate * s
            back_up[h, at, :] = back_up[h, at, :] * s * (1.0 + gate * (1.0 - s))

    for w in range(2, 3):
        group(w, planes - 1)

    @pl.loop(0, 2)
    def _(h):
        back = 0.5 * wide_dot(toks[2, h], weights[2])
        fwd_gate[h] = back
        gate_diff[pl.ds(pl.multiple_of(h * slab, slab), slab), :] = (back * back_up[h]).astype(jnp.bfloat16)
        up_diff[pl.ds(pl.multiple_of(h * slab, slab), slab), :] = (back * back_gate[h]).astype(jnp.bfloat16)

    def grad_copy(step):
        to = (fs + step) % n_fs
        return remote(grad_send.at[to], grad_recv.at[fs], grad_send_sem.at[to], grad_recv_sem.at[fs], (to, core))

    diff_turned = gate_diff[...].T

    for step in range(planes):
        there = (level + step + 1) % planes
        cols = pl.ds(pl.multiple_of(there * plane * depth, plane * depth), plane * depth)
        product = jnp.dot(diff_turned[:, :slab], toks[0, 0, :, cols], preferred_element_type=jnp.float32)
        product = product + jnp.dot(diff_turned[:, slab:], toks[0, 1, :, cols], preferred_element_type=jnp.float32)
        product = product.astype(jnp.bfloat16)
        for q in range(plane):
            grad_send[there * plane + q] = product[:, q * depth : (q + 1) * depth]
        for q in range(plane):
            to = there * plane + q

            @pl.when(to != fs)
            def _():
                remote(grad_send.at[to], grad_recv.at[fs], grad_send_sem.at[to], grad_recv_sem.at[fs], (to, core)).start()

    grad_recv[fs] = grad_send[fs]

    def cross(k):
        return remote(part.at[k, 1 - core], crossed.at[k], cross_sem.at[k, 0], cross_sem.at[k, 1], sibling)

    def join(k, step):
        q = (place + step) % plane
        return remote(joined.at[k, q], gathered.at[k, place], join_send.at[k, step], join_recv.at[k, place], (level * plane + q, core))

    strip = 512

    def partial(k, h):
        rows_at = pl.ds(pl.multiple_of(h * slab, slab), slab)

        @pl.loop(0, width // strip)
        def _(t):
            at = pl.ds(pl.multiple_of(t * strip, strip), strip)
            if k == 0:
                value = jnp.dot(hidden[h], weights[2, :, at], preferred_element_type=jnp.float32)
            else:
                value = jnp.dot(gate_diff[rows_at, :], weights[0, :, at], preferred_element_type=jnp.float32)
                value = value + jnp.dot(up_diff[rows_at, :], weights[1, :, at], preferred_element_type=jnp.float32)
            part[k, h, :, at] = value.astype(jnp.bfloat16)

    for k in range(2):
        partial(k, 1 - core)
        cross(k).start()
    for k in range(2):
        partial(k, core)
    for k in range(2):
        cross(k).wait_recv()
        for step in range(plane):
            q = (place + step + 1) % plane
            at = pl.ds(pl.multiple_of(q * half, half), half)
            total = part[k, core, at, :].astype(jnp.float32) + crossed[k, at, :].astype(jnp.float32)
            joined[k, q] = total.astype(jnp.bfloat16)
            if step < plane - 1:
                join(k, step + 1).start()
    for k in range(2):
        gathered[k, place] = joined[k, place]

    mine = pl.ds(pl.multiple_of(core * half, half), half)

    def last(k):
        out = (fwd_out, back_out)[k]
        return remote(out.at[mine, :], out.at[mine, :], last_sem.at[k, 0], last_sem.at[k, 1], sibling)

    def joined_in(k):
        for step in range(1, plane):
            q = (place + step) % plane
            remote(joined.at[k, q], gathered.at[k, q], join_send.at[k, 0], join_recv.at[k, q], sibling).wait_recv()

    def total_of(k, at):
        value = gathered[k, 0, at, :].astype(jnp.float32)
        for q in range(1, plane):
            value = value + gathered[k, q, at, :].astype(jnp.float32)
        return value

    small = 16
    joined_in(0)
    for r in range(half // small):
        at = pl.ds(r * small, small)
        fwd_out[pl.ds(pl.multiple_of(core * half + r * small, small), small), :] = (0.5 * total_of(0, at)).astype(jnp.bfloat16)
    joined_in(1)
    for r in range(half // small):
        at = pl.ds(r * small, small)
        there = pl.ds(pl.multiple_of(core * half + r * small, small), small)
        values = tokens_ref[there, :].astype(jnp.float32)
        factor = lax.rsqrt(jnp.mean(values * values, axis=-1, keepdims=True) + norm_eps)
        scaled = total_of(1, at) * gain_ref[...]
        cubed = factor * factor * factor
        back_out[there, :] = (
            factor * scaled - values * cubed * jnp.mean(scaled * values, axis=-1, keepdims=True)
        ).astype(jnp.bfloat16)
    for k in range(2):
        last(k).start()

    for step in range(1, n_fs):
        src = (fs + step) % n_fs
        remote(grad_send.at[src], grad_recv.at[src], grad_send_sem.at[src], grad_recv_sem.at[src], sibling).wait_recv()
    for q in range(plane):
        total = grad_recv[q].astype(jnp.float32)
        for z in range(1, planes):
            total = total + grad_recv[z * plane + q].astype(jnp.float32)
        grad_cols[q * rows : (q + 1) * rows, :] = total

    @pl.loop(0, grad_cols.shape[0] // 128)
    def _(t):
        at = pl.ds(pl.multiple_of(t * 128, 128), 128)
        sum_out[:, at] = sum_ref[:, at] + grad_cols[at, :].T

    for w in range(3):
        for step in range(1, plane):
            staged(w, step).wait_send()
        for way in (1, -1):
            for d in range(planes - 1):
                other = level - way * d

                @pl.when(jnp.logical_and(can[way], jnp.logical_and(other >= 0, other < planes)))
                def _():
                    @pl.loop(0, plane)
                    def _(q):
                        src = other * plane + q
                        hop(w, src, block(w, src), way).wait_send()

    for a in range(3):
        for step in range(1, plane):
            tok_copy(a, step).wait_send()
            relay(a, (place + step) % plane).wait_send()
    for step in range(1, n_fs):
        grad_copy(step).wait_send()
    for k in range(2):
        cross(k).wait_send()
        for step in range(1, plane):
            join(k, step).wait_send()
        last(k).wait()


def fused_shards(
    planes, plane, fwd_tokens, back_tokens, out_grad, norm_gain, gate_weight, up_weight, down_weight, gate_grad_sum
):
    tokens, width = fwd_tokens.shape
    depth, cols = gate_weight.shape
    rows = cols // plane
    half = tokens // 2
    slab = half * plane
    n_fs = planes * plane
    fwd_normed = normalize(fwd_tokens, norm_gain)[2]
    back_normed = normalize(back_tokens, norm_gain)[2]
    narrow, full = jnp.bfloat16, jnp.float32
    dma = pltpu.SemaphoreType.DMA
    vmem = pl.BlockSpec(memory_space=pltpu.VMEM)
    return pl.pallas_call(
        functools.partial(layer_kernel, planes, plane),
        out_shape=(
            jax.ShapeDtypeStruct((tokens, width), narrow),
            jax.ShapeDtypeStruct((tokens, width), narrow),
            jax.ShapeDtypeStruct((depth, cols), full),
        ),
        in_specs=[vmem] * 9,
        out_specs=(vmem,) * 3,
        scratch_shapes=[
            pltpu.VMEM((3, 2, slab, width), narrow),
            pltpu.VMEM((3, rows, width), narrow),
            pltpu.VMEM((2, slab, rows), full),
            pltpu.VMEM((2, slab, rows), full),
            pltpu.VMEM((2, slab, rows), full),
            pltpu.VMEM((2, slab, rows), full),
            pltpu.VMEM((2, slab, rows), narrow),
            pltpu.VMEM((2 * slab, rows), narrow),
            pltpu.VMEM((2 * slab, rows), narrow),
            pltpu.VMEM((2, 2, slab, width), narrow),
            pltpu.VMEM((2, slab, width), narrow),
            pltpu.VMEM((2, plane, half, width), narrow),
            pltpu.VMEM((2, plane, half, width), narrow),
            pltpu.VMEM((n_fs, rows, depth), narrow),
            pltpu.VMEM((n_fs, rows, depth), narrow),
            pltpu.VMEM((cols, depth), full),
            dma((3, plane)),
            dma((3, n_fs)),
            dma((3, n_fs)),
            dma((3, n_fs)),
            dma((3, plane)),
            dma((3, plane)),
            dma((3, plane)),
            dma((3, plane)),
            dma((n_fs,)),
            dma((n_fs,)),
            dma((2, 2)),
            dma((2, plane)),
            dma((2, plane)),
            dma((2, 2)),
        ],
        compiler_params=pltpu.CompilerParams(
            collective_id=0, has_side_effects=True, vmem_limit_bytes=56 * 2**20
        ),
    )(
        fwd_normed, back_normed, out_grad, back_tokens, norm_gain.reshape(1, width),
        gate_weight.T, up_weight.T, down_weight.T, gate_grad_sum,
    )


def square_side(count):
    side = 1
    while side * side * 4 <= count:
        side *= 2
    return side


def body_for(mesh):
    n_fs, plane = mesh.shape["fs"], square_side(mesh.shape["fs"])

    def body(*args):
        tokens, width = args[0].shape
        depth, cols = args[4].shape
        fits = (
            mesh.shape["tp"] == 2 and n_fs % plane == 0 and n_fs // plane >= 3 and plane >= 2
            and depth == 128 and cols % (plane * 16) == 0 and cols % 128 == 0
            and tokens % 128 == 0 and width % 512 == 0
        )
        if not fits:
            return shards(*args)
        return fused_shards(n_fs // plane, plane, *args)

    return body


def solution(mesh):
    in_specs = (
        P("fs", None),
        P("fs", None),
        P("fs", None),
        P(),
        P("fs", "tp"),
        P("fs", "tp"),
        P("fs", "tp"),
        P("fs", "tp"),
    )
    out_specs = (P("fs", None), P("fs", None), P("fs", "tp"))
    return jax.shard_map(body_for(mesh), mesh=mesh, in_specs=in_specs, out_specs=out_specs, check_vma=False)
```

```python
import functools

import jax
import jax.numpy as jnp
from jax import lax
from jax.experimental import pallas as pl
from jax.experimental.pallas import tpu as pltpu
from jax.sharding import PartitionSpec as P

norm_eps = 0.25


def normalize(tokens, norm_gain):
    values = tokens.astype(jnp.float32)
    factor = lax.rsqrt(jnp.mean(values * values, axis=-1, keepdims=True) + norm_eps)
    return (values, factor, (values * factor * norm_gain).astype(jnp.bfloat16))


def shards(
    fwd_tokens, back_tokens, out_grad, norm_gain, gate_weight, up_weight, down_weight, gate_grad_sum
):
    fwd_normed = normalize(fwd_tokens, norm_gain)[2]
    columns = fwd_normed
    gate_pre = jnp.dot(
        columns,
        lax.all_gather(gate_weight, "fs", axis=0, tiled=True),
        preferred_element_type=jnp.float32,
    )
    up_pre = jnp.dot(
        columns,
        lax.all_gather(up_weight, "fs", axis=0, tiled=True),
        preferred_element_type=jnp.float32,
    )
    hidden = (gate_pre * jax.nn.sigmoid(gate_pre) * up_pre).astype(jnp.bfloat16)
    partial_value = jnp.dot(
        hidden,
        lax.all_gather(down_weight, "fs", axis=0, tiled=True).T,
        preferred_element_type=jnp.float32,
    )
    summed = lax.psum(partial_value.astype(jnp.bfloat16), "tp").astype(jnp.float32)
    fwd_out = (0.5 * summed).astype(jnp.bfloat16)
    gate_whole = lax.all_gather(gate_weight, "fs", axis=0, tiled=True)
    up_whole = lax.all_gather(up_weight, "fs", axis=0, tiled=True)
    down_whole = lax.all_gather(down_weight, "fs", axis=0, tiled=True)
    values, factor, back_normed = normalize(back_tokens, norm_gain)
    gate_pre = jnp.dot(back_normed, gate_whole, preferred_element_type=jnp.float32)
    up_pre = jnp.dot(back_normed, up_whole, preferred_element_type=jnp.float32)
    sigmoid_gate = jax.nn.sigmoid(gate_pre)
    back_hidden = 0.5 * jnp.dot(out_grad, down_whole, preferred_element_type=jnp.float32)
    gate_diff = (
        back_hidden * up_pre * sigmoid_gate * (1.0 + gate_pre * (1.0 - sigmoid_gate))
    ).astype(jnp.bfloat16)
    up_diff = (back_hidden * gate_pre * sigmoid_gate).astype(jnp.bfloat16)
    columns = back_normed
    gate_grad_out = gate_grad_sum + lax.psum_scatter(
        jnp.dot(columns.T, gate_diff, preferred_element_type=jnp.float32),
        "fs",
        scatter_dimension=0,
        tiled=True,
    )
    partial_diff = jnp.dot(gate_diff, gate_whole.T, preferred_element_type=jnp.float32)
    partial_diff = partial_diff + jnp.dot(up_diff, up_whole.T, preferred_element_type=jnp.float32)
    normed_diff = lax.psum(partial_diff.astype(jnp.bfloat16), "tp").astype(jnp.float32)
    scaled = normed_diff * norm_gain
    cubed = factor * factor * factor
    back_grad = (
        factor * scaled - values * cubed * jnp.mean(scaled * values, axis=-1, keepdims=True)
    ).astype(jnp.bfloat16)
    back_grad, gate_grad_out = (back_grad, gate_grad_out)
    return (fwd_out, back_grad, gate_grad_out)


MESH = pl.DeviceIdType.MESH


def wide_dot(a, b):
    return lax.dot_general(a, b, (((1,), (1,)), ((), ())), preferred_element_type=jnp.float32)


def layer_kernel(
    planes, plane, fwd_ref, back_ref, grad_ref, tokens_ref, gain_ref, gate_ref, up_ref, down_ref, sum_ref,
    fwd_out, back_out, sum_out,
    toks, weights, fwd_gate, fwd_up, back_gate, back_up, hidden, gate_diff, up_diff,
    part, crossed, joined, gathered, grad_send, lifted, dropped, grad_recv, grad_cols,
    stage_sem, weight_sem, up_sem, down_sem, tok_send, tok_recv, relay_send, relay_recv,
    lift_send, lift_recv, drop_send, drop_recv, turn_send, turn_recv, cross_sem, join_send, join_recv, last_sem,
):
    n_fs = planes * plane
    fs, core = lax.axis_index("fs"), lax.axis_index("tp")
    level, place = fs // plane, fs % plane
    sibling = (fs, 1 - core)
    rows = weights.shape[1]
    depth = gate_ref.shape[1]
    half = fwd_ref.shape[0] // 2
    slab = half * plane
    width = fwd_ref.shape[1]

    barrier = pltpu.get_barrier_semaphore()
    for step in range(1, n_fs):
        pl.semaphore_signal(barrier, inc=1, device_id=((fs + step) % n_fs, core), device_id_type=MESH)
    pl.semaphore_signal(barrier, inc=1, device_id=sibling, device_id_type=MESH)
    pl.semaphore_wait(barrier, n_fs)

    def remote(src, dst, send, recv, device):
        return pltpu.make_async_remote_copy(
            src_ref=src, dst_ref=dst, send_sem=send, recv_sem=recv, device_id=device, device_id_type=MESH
        )

    own = (gate_ref, up_ref, down_ref)

    def own_block(w, q):
        return own[w].at[pl.ds(pl.multiple_of(q * rows, rows), rows), :]

    def block(w, src):
        return weights.at[w, :, pl.ds(pl.multiple_of(src * depth, depth), depth)]

    def staged(w, step):
        q = (place + step) % plane
        return remote(own_block(w, q), block(w, fs), stage_sem.at[w, step], weight_sem.at[w, fs], (level * plane + q, core))

    def arrived(w, src):
        remote(block(w, src), block(w, src), stage_sem.at[w, 0], weight_sem.at[w, src], sibling).wait_recv()

    def hop(w, src, source, step):
        sem = up_sem if step > 0 else down_sem
        return remote(source, block(w, src), sem.at[w, src], weight_sem.at[w, src], ((fs + step * plane + n_fs) % n_fs, core))

    can = {1: level < planes - 1, -1: level > 0}

    def send_on(w, src, source, step):
        @pl.when(can[step])
        def _():
            hop(w, src, source, step).start()

    token_refs = (back_ref, fwd_ref, grad_ref)

    def tok_block(a, h, q):
        return toks.at[a, h, pl.ds(pl.multiple_of(q * half, half), half), :]

    def tok_copy(a, step):
        q = (place + step) % plane
        return remote(
            token_refs[a].at[pl.ds(pl.multiple_of(core * half, half), half), :],
            tok_block(a, core, place), tok_send.at[a, step], tok_recv.at[a, place], (level * plane + q, core),
        )

    def tok_arrived(a, q):
        remote(tok_block(a, core, q), tok_block(a, core, q), tok_send.at[a, 0], tok_recv.at[a, q], sibling).wait_recv()

    def relay(a, q):
        return remote(tok_block(a, core, q), tok_block(a, core, q), relay_send.at[a, q], relay_recv.at[a, q], sibling)

    def relayed(a, q):
        remote(tok_block(a, 1 - core, q), tok_block(a, 1 - core, q), relay_send.at[a, q], relay_recv.at[a, q], sibling).wait_recv()

    for w in range(3):
        for step in range(1, plane):
            staged(w, step).start()
        for step in (1, -1):
            send_on(w, fs, own_block(w, place), step)
    for a in range(3):
        for step in range(1, plane):
            tok_copy(a, step).start()
    for w in range(3):
        weights[w, :, pl.ds(pl.multiple_of(fs * depth, depth), depth)] = own[w][pl.ds(pl.multiple_of(place * rows, rows), rows), :]
    for a in range(3):
        for h in range(2):
            toks[a, h, pl.ds(pl.multiple_of(place * half, half), half), :] = token_refs[a][pl.ds(h * half, half), :]

    def group(w, d):
        if d == 0:
            for step in range(1, plane):
                src = level * plane + (place + step) % plane
                arrived(w, src)
                for way in (1, -1):
                    send_on(w, src, block(w, src), way)
            return
        for way in (1, -1):
            other = level - way * d

            @pl.when(jnp.logical_and(other >= 0, other < planes))
            def _():
                @pl.loop(0, plane)
                def _(q):
                    src = other * plane + q
                    arrived(w, src)
                    send_on(w, src, block(w, src), way)

    def relays(a):
        for step in range(1, plane):
            q = (place + step) % plane
            tok_arrived(a, q)
            relay(a, q).start()

    def relays_in(a):
        for step in range(1, plane):
            relayed(a, (place + step) % plane)

    def project(a, w, out):
        @pl.loop(0, 2)
        def _(h):
            out[h] = wide_dot(toks[a, h], weights[w])

    for d in range(planes - 1):
        for w in range(3):
            group(w, d)
    for a in range(3):
        relays(a)
    for a in range(3):
        relays_in(a)
    group(0, planes - 1)
    project(0, 0, back_gate)
    project(1, 0, fwd_gate)
    group(1, planes - 1)
    project(0, 1, back_up)
    project(1, 1, fwd_up)

    piece = 64

    @pl.loop(0, 2)
    def _(h):
        @pl.loop(0, slab // piece)
        def _(r):
            at = pl.ds(pl.multiple_of(r * piece, piece), piece)
            gate = fwd_gate[h, at, :]
            hidden[h, at, :] = (gate * jax.nn.sigmoid(gate) * fwd_up[h, at, :]).astype(jnp.bfloat16)
            gate = back_gate[h, at, :]
            s = jax.nn.sigmoid(gate)
            back_gate[h, at, :] = gate * s
            back_up[h, at, :] = back_up[h, at, :] * s * (1.0 + gate * (1.0 - s))

    group(2, planes - 1)

    @pl.loop(0, 2)
    def _(h):
        back = 0.5 * wide_dot(toks[2, h], weights[2])
        fwd_gate[h] = back
        gate_diff[pl.ds(pl.multiple_of(h * slab, slab), slab), :] = (back * back_up[h]).astype(jnp.bfloat16)
        up_diff[pl.ds(pl.multiple_of(h * slab, slab), slab), :] = (back * back_gate[h]).astype(jnp.bfloat16)

    def grad_hop(b, way):
        sends, recvs, lands = (lift_send, lift_recv, lifted) if way > 0 else (drop_send, drop_recv, dropped)
        to = (fs + way * plane + n_fs) % n_fs
        return remote(grad_send.at[b], lands.at[b], sends.at[b], recvs.at[b], (to, core))

    diff_turned = gate_diff[...].T

    for step in range(planes):
        there = jnp.where(2 * level < planes, planes - 1 - step, step)
        cols = pl.ds(pl.multiple_of(there * plane * depth, plane * depth), plane * depth)
        product = jnp.dot(diff_turned[:, :slab], toks[0, 0, :, cols], preferred_element_type=jnp.float32)
        product = product + jnp.dot(diff_turned[:, slab:], toks[0, 1, :, cols], preferred_element_type=jnp.float32)
        product = product.astype(jnp.bfloat16)
        for q in range(plane):
            grad_send[there * plane + q] = product[:, q * depth : (q + 1) * depth]
        for way, first in ((1, 0), (-1, planes - 1)):

            @pl.when(jnp.logical_and(level == first, there != first))
            def _():
                for q in range(plane):
                    grad_hop(there * plane + q, way).start()

    def serve(i):
        for way in (1, -1):
            lands = lifted if way > 0 else dropped
            there = planes - 1 - i if way > 0 else i
            left = (there - level) * way

            @pl.when(jnp.logical_and(can[-way], left >= 0))
            def _():
                @pl.loop(0, plane)
                def _(q):
                    b = there * plane + q
                    grad_hop(b, way).wait_recv()
                    total = grad_send[b].astype(jnp.float32) + lands[b].astype(jnp.float32)
                    grad_send[b] = total.astype(jnp.bfloat16)

                    @pl.when(left > 0)
                    def _():
                        grad_hop(b, way).start()

    def turn(step):
        q = (place + step) % plane
        return remote(grad_send.at[level * plane + q], grad_recv.at[place], turn_send.at[step], turn_recv.at[place], (level * plane + q, core))

    def cross(k):
        return remote(part.at[k, 1 - core], crossed.at[k], cross_sem.at[k, 0], cross_sem.at[k, 1], sibling)

    def join(k, step):
        q = (place + step) % plane
        return remote(joined.at[k, q], gathered.at[k, place], join_send.at[k, step], join_recv.at[k, place], (level * plane + q, core))

    strip = 512

    def partial(k, h):
        rows_at = pl.ds(pl.multiple_of(h * slab, slab), slab)

        @pl.loop(0, width // strip)
        def _(t):
            at = pl.ds(pl.multiple_of(t * strip, strip), strip)
            if k == 0:
                value = jnp.dot(hidden[h], weights[2, :, at], preferred_element_type=jnp.float32)
            else:
                value = jnp.dot(gate_diff[rows_at, :], weights[0, :, at], preferred_element_type=jnp.float32)
                value = value + jnp.dot(up_diff[rows_at, :], weights[1, :, at], preferred_element_type=jnp.float32)
            part[k, h, :, at] = value.astype(jnp.bfloat16)

    for k in range(2):
        partial(k, 1 - core)
        cross(k).start()
    for k in range(2):
        partial(k, core)
    for k in range(2):
        cross(k).wait_recv()
        for step in range(plane):
            q = (place + step + 1) % plane
            at = pl.ds(pl.multiple_of(q * half, half), half)
            total = part[k, core, at, :].astype(jnp.float32) + crossed[k, at, :].astype(jnp.float32)
            joined[k, q] = total.astype(jnp.bfloat16)
            if step < plane - 1:
                join(k, step + 1).start()
    for i in range(planes):
        serve(i)
    for step in range(1, plane):
        turn(step).start()
    grad_recv[place] = grad_send[fs]
    for k in range(2):
        gathered[k, place] = joined[k, place]

    mine = pl.ds(pl.multiple_of(core * half, half), half)

    def last(k):
        out = (fwd_out, back_out)[k]
        return remote(out.at[mine, :], out.at[mine, :], last_sem.at[k, 0], last_sem.at[k, 1], sibling)

    def joined_in(k):
        for step in range(1, plane):
            q = (place + step) % plane
            remote(joined.at[k, q], gathered.at[k, q], join_send.at[k, 0], join_recv.at[k, q], sibling).wait_recv()

    def total_of(k, at):
        value = gathered[k, 0, at, :].astype(jnp.float32)
        for q in range(1, plane):
            value = value + gathered[k, q, at, :].astype(jnp.float32)
        return value

    small = 16
    joined_in(0)
    for r in range(half // small):
        at = pl.ds(r * small, small)
        fwd_out[pl.ds(pl.multiple_of(core * half + r * small, small), small), :] = (0.5 * total_of(0, at)).astype(jnp.bfloat16)
    joined_in(1)
    for r in range(half // small):
        at = pl.ds(r * small, small)
        there = pl.ds(pl.multiple_of(core * half + r * small, small), small)
        values = tokens_ref[there, :].astype(jnp.float32)
        factor = lax.rsqrt(jnp.mean(values * values, axis=-1, keepdims=True) + norm_eps)
        scaled = total_of(1, at) * gain_ref[...]
        cubed = factor * factor * factor
        back_out[there, :] = (
            factor * scaled - values * cubed * jnp.mean(scaled * values, axis=-1, keepdims=True)
        ).astype(jnp.bfloat16)
    for k in range(2):
        last(k).start()

    for step in range(1, plane):
        q = (place + step) % plane
        remote(grad_send.at[fs], grad_recv.at[q], turn_send.at[0], turn_recv.at[q], sibling).wait_recv()
    for q in range(plane):
        grad_cols[q * rows : (q + 1) * rows, :] = grad_recv[q].astype(jnp.float32)

    @pl.loop(0, grad_cols.shape[0] // 128)
    def _(t):
        at = pl.ds(pl.multiple_of(t * 128, 128), 128)
        sum_out[:, at] = sum_ref[:, at] + grad_cols[at, :].T

    for w in range(3):
        for step in range(1, plane):
            staged(w, step).wait_send()
        for way in (1, -1):
            for d in range(planes - 1):
                other = level - way * d

                @pl.when(jnp.logical_and(can[way], jnp.logical_and(other >= 0, other < planes)))
                def _():
                    @pl.loop(0, plane)
                    def _(q):
                        src = other * plane + q
                        hop(w, src, block(w, src), way).wait_send()

    for a in range(3):
        for step in range(1, plane):
            tok_copy(a, step).wait_send()
            relay(a, (place + step) % plane).wait_send()
    for step in range(1, plane):
        turn(step).wait_send()
    for way in (1, -1):

        @pl.when(can[way])
        def _():
            @pl.loop(0, planes)
            def _(there):
                @pl.when((there - level) * way > 0)
                def _():
                    @pl.loop(0, plane)
                    def _(q):
                        grad_hop(there * plane + q, way).wait_send()

    for k in range(2):
        cross(k).wait_send()
        for step in range(1, plane):
            join(k, step).wait_send()
        last(k).wait()


def fused_shards(
    planes, plane, fwd_tokens, back_tokens, out_grad, norm_gain, gate_weight, up_weight, down_weight, gate_grad_sum
):
    tokens, width = fwd_tokens.shape
    depth, cols = gate_weight.shape
    rows = cols // plane
    half = tokens // 2
    slab = half * plane
    n_fs = planes * plane
    fwd_normed = normalize(fwd_tokens, norm_gain)[2]
    back_normed = normalize(back_tokens, norm_gain)[2]
    narrow, full = jnp.bfloat16, jnp.float32
    dma = pltpu.SemaphoreType.DMA
    vmem = pl.BlockSpec(memory_space=pltpu.VMEM)
    return pl.pallas_call(
        functools.partial(layer_kernel, planes, plane),
        out_shape=(
            jax.ShapeDtypeStruct((tokens, width), narrow),
            jax.ShapeDtypeStruct((tokens, width), narrow),
            jax.ShapeDtypeStruct((depth, cols), full),
        ),
        in_specs=[vmem] * 9,
        out_specs=(vmem,) * 3,
        scratch_shapes=[
            pltpu.VMEM((3, 2, slab, width), narrow),
            pltpu.VMEM((3, rows, width), narrow),
            pltpu.VMEM((2, slab, rows), full),
            pltpu.VMEM((2, slab, rows), full),
            pltpu.VMEM((2, slab, rows), full),
            pltpu.VMEM((2, slab, rows), full),
            pltpu.VMEM((2, slab, rows), narrow),
            pltpu.VMEM((2 * slab, rows), narrow),
            pltpu.VMEM((2 * slab, rows), narrow),
            pltpu.VMEM((2, 2, slab, width), narrow),
            pltpu.VMEM((2, slab, width), narrow),
            pltpu.VMEM((2, plane, half, width), narrow),
            pltpu.VMEM((2, plane, half, width), narrow),
            pltpu.VMEM((n_fs, rows, depth), narrow),
            pltpu.VMEM((n_fs, rows, depth), narrow),
            pltpu.VMEM((n_fs, rows, depth), narrow),
            pltpu.VMEM((plane, rows, depth), narrow),
            pltpu.VMEM((cols, depth), full),
            dma((3, plane)),
            dma((3, n_fs)),
            dma((3, n_fs)),
            dma((3, n_fs)),
            dma((3, plane)),
            dma((3, plane)),
            dma((3, plane)),
            dma((3, plane)),
            dma((n_fs,)),
            dma((n_fs,)),
            dma((n_fs,)),
            dma((n_fs,)),
            dma((plane,)),
            dma((plane,)),
            dma((2, 2)),
            dma((2, plane)),
            dma((2, plane)),
            dma((2, 2)),
        ],
        compiler_params=pltpu.CompilerParams(
            collective_id=0, has_side_effects=True, vmem_limit_bytes=56 * 2**20
        ),
    )(
        fwd_normed, back_normed, out_grad, back_tokens, norm_gain.reshape(1, width),
        gate_weight.T, up_weight.T, down_weight.T, gate_grad_sum,
    )


def square_side(count):
    side = 1
    while side * side * 4 <= count:
        side *= 2
    return side


def body_for(mesh):
    n_fs, plane = mesh.shape["fs"], square_side(mesh.shape["fs"])

    def body(*args):
        tokens, width = args[0].shape
        depth, cols = args[4].shape
        fits = (
            mesh.shape["tp"] == 2 and n_fs % plane == 0 and n_fs // plane >= 3 and plane >= 2
            and depth == 128 and cols % (plane * 16) == 0 and cols % 128 == 0
            and tokens % 128 == 0 and width % 512 == 0
        )
        if not fits:
            return shards(*args)
        return fused_shards(n_fs // plane, plane, *args)

    return body


def solution(mesh):
    in_specs = (
        P("fs", None),
        P("fs", None),
        P("fs", None),
        P(),
        P("fs", "tp"),
        P("fs", "tp"),
        P("fs", "tp"),
        P("fs", "tp"),
    )
    out_specs = (P("fs", None), P("fs", None), P("fs", "tp"))
    return jax.shard_map(body_for(mesh), mesh=mesh, in_specs=in_specs, out_specs=out_specs, check_vma=False)
```

```python
import functools

import jax
import jax.numpy as jnp
from jax import lax
from jax.experimental import pallas as pl
from jax.experimental.pallas import tpu as pltpu
from jax.sharding import PartitionSpec as P

norm_eps = 0.25


def normalize(tokens, norm_gain):
    values = tokens.astype(jnp.float32)
    factor = lax.rsqrt(jnp.mean(values * values, axis=-1, keepdims=True) + norm_eps)
    return (values, factor, (values * factor * norm_gain).astype(jnp.bfloat16))


def shards(
    fwd_tokens, back_tokens, out_grad, norm_gain, gate_weight, up_weight, down_weight, gate_grad_sum
):
    fwd_normed = normalize(fwd_tokens, norm_gain)[2]
    columns = fwd_normed
    gate_pre = jnp.dot(
        columns,
        lax.all_gather(gate_weight, "fs", axis=0, tiled=True),
        preferred_element_type=jnp.float32,
    )
    up_pre = jnp.dot(
        columns,
        lax.all_gather(up_weight, "fs", axis=0, tiled=True),
        preferred_element_type=jnp.float32,
    )
    hidden = (gate_pre * jax.nn.sigmoid(gate_pre) * up_pre).astype(jnp.bfloat16)
    partial_value = jnp.dot(
        hidden,
        lax.all_gather(down_weight, "fs", axis=0, tiled=True).T,
        preferred_element_type=jnp.float32,
    )
    summed = lax.psum(partial_value.astype(jnp.bfloat16), "tp").astype(jnp.float32)
    fwd_out = (0.5 * summed).astype(jnp.bfloat16)
    gate_whole = lax.all_gather(gate_weight, "fs", axis=0, tiled=True)
    up_whole = lax.all_gather(up_weight, "fs", axis=0, tiled=True)
    down_whole = lax.all_gather(down_weight, "fs", axis=0, tiled=True)
    values, factor, back_normed = normalize(back_tokens, norm_gain)
    gate_pre = jnp.dot(back_normed, gate_whole, preferred_element_type=jnp.float32)
    up_pre = jnp.dot(back_normed, up_whole, preferred_element_type=jnp.float32)
    sigmoid_gate = jax.nn.sigmoid(gate_pre)
    back_hidden = 0.5 * jnp.dot(out_grad, down_whole, preferred_element_type=jnp.float32)
    gate_diff = (
        back_hidden * up_pre * sigmoid_gate * (1.0 + gate_pre * (1.0 - sigmoid_gate))
    ).astype(jnp.bfloat16)
    up_diff = (back_hidden * gate_pre * sigmoid_gate).astype(jnp.bfloat16)
    columns = back_normed
    gate_grad_out = gate_grad_sum + lax.psum_scatter(
        jnp.dot(columns.T, gate_diff, preferred_element_type=jnp.float32),
        "fs",
        scatter_dimension=0,
        tiled=True,
    )
    partial_diff = jnp.dot(gate_diff, gate_whole.T, preferred_element_type=jnp.float32)
    partial_diff = partial_diff + jnp.dot(up_diff, up_whole.T, preferred_element_type=jnp.float32)
    normed_diff = lax.psum(partial_diff.astype(jnp.bfloat16), "tp").astype(jnp.float32)
    scaled = normed_diff * norm_gain
    cubed = factor * factor * factor
    back_grad = (
        factor * scaled - values * cubed * jnp.mean(scaled * values, axis=-1, keepdims=True)
    ).astype(jnp.bfloat16)
    back_grad, gate_grad_out = (back_grad, gate_grad_out)
    return (fwd_out, back_grad, gate_grad_out)


MESH = pl.DeviceIdType.MESH


def wide_dot(a, b):
    return lax.dot_general(a, b, (((1,), (1,)), ((), ())), preferred_element_type=jnp.float32)


def layer_kernel(
    planes, plane, fwd_ref, tokens_ref, grad_ref, gain_ref, gate_ref, up_ref, down_ref, sum_ref,
    fwd_out, back_out, sum_out,
    turned, normed, toks, weights, fwd_gate, fwd_up, back_gate, back_up, hidden, gate_diff, up_diff,
    part, crossed, joined, gathered, grad_send, lifted, dropped, grad_recv, grad_cols,
    stage_sem, weight_sem, up_sem, down_sem, tok_send, tok_recv, relay_send, relay_recv,
    lift_send, lift_recv, drop_send, drop_recv, turn_send, turn_recv, cross_sem, join_send, join_recv, last_sem,
):
    n_fs = planes * plane
    fs, core = lax.axis_index("fs"), lax.axis_index("tp")
    level, place = fs // plane, fs % plane
    sibling = (fs, 1 - core)
    rows = weights.shape[1]
    depth = gate_ref.shape[0]
    half = fwd_ref.shape[0] // 2
    slab = half * plane
    width = fwd_ref.shape[1]

    barrier = pltpu.get_barrier_semaphore()
    for step in range(1, n_fs):
        pl.semaphore_signal(barrier, inc=1, device_id=((fs + step) % n_fs, core), device_id_type=MESH)
    pl.semaphore_signal(barrier, inc=1, device_id=sibling, device_id_type=MESH)

    @pl.loop(0, turned.shape[1] // 128)
    def _(t):
        at = pl.ds(pl.multiple_of(t * 128, 128), 128)
        turned[0, at, :] = gate_ref[:, at].T
        turned[1, at, :] = up_ref[:, at].T
        turned[2, at, :] = down_ref[:, at].T

    @pl.loop(0, fwd_ref.shape[0] // 16)
    def _(r):
        at = pl.ds(pl.multiple_of(r * 16, 16), 16)
        for a, ref in ((0, tokens_ref), (1, fwd_ref)):
            normed[a, at, :] = normalize(ref[at, :], gain_ref[...])[2]

    pl.semaphore_wait(barrier, n_fs)

    def remote(src, dst, send, recv, device):
        return pltpu.make_async_remote_copy(
            src_ref=src, dst_ref=dst, send_sem=send, recv_sem=recv, device_id=device, device_id_type=MESH
        )

    def own_block(w, q):
        return turned.at[w, pl.ds(pl.multiple_of(q * rows, rows), rows), :]

    def block(w, src):
        return weights.at[w, :, pl.ds(pl.multiple_of(src * depth, depth), depth)]

    def staged(w, step):
        q = (place + step) % plane
        return remote(own_block(w, q), block(w, fs), stage_sem.at[w, step], weight_sem.at[w, fs], (level * plane + q, core))

    def arrived(w, src):
        remote(block(w, src), block(w, src), stage_sem.at[w, 0], weight_sem.at[w, src], sibling).wait_recv()

    def hop(w, src, source, step):
        sem = up_sem if step > 0 else down_sem
        return remote(source, block(w, src), sem.at[w, src], weight_sem.at[w, src], ((fs + step * plane + n_fs) % n_fs, core))

    can = {1: level < planes - 1, -1: level > 0}

    def send_on(w, src, source, step):
        @pl.when(can[step])
        def _():
            hop(w, src, source, step).start()

    def token_rows(a, at):
        return grad_ref.at[at, :] if a == 2 else normed.at[a, at, :]

    def tok_block(a, h, q):
        return toks.at[a, h, pl.ds(pl.multiple_of(q * half, half), half), :]

    def tok_copy(a, step):
        q = (place + step) % plane
        return remote(
            token_rows(a, pl.ds(pl.multiple_of(core * half, half), half)),
            tok_block(a, core, place), tok_send.at[a, step], tok_recv.at[a, place], (level * plane + q, core),
        )

    def tok_arrived(a, q):
        remote(tok_block(a, core, q), tok_block(a, core, q), tok_send.at[a, 0], tok_recv.at[a, q], sibling).wait_recv()

    def relay(a, q):
        return remote(tok_block(a, core, q), tok_block(a, core, q), relay_send.at[a, q], relay_recv.at[a, q], sibling)

    def relayed(a, q):
        remote(tok_block(a, 1 - core, q), tok_block(a, 1 - core, q), relay_send.at[a, q], relay_recv.at[a, q], sibling).wait_recv()

    for w in range(3):
        for step in range(1, plane):
            staged(w, step).start()
        for step in (1, -1):
            send_on(w, fs, own_block(w, place), step)
    for a in range(3):
        for step in range(1, plane):
            tok_copy(a, step).start()
    for w in range(3):
        weights[w, :, pl.ds(pl.multiple_of(fs * depth, depth), depth)] = turned[w, pl.ds(pl.multiple_of(place * rows, rows), rows), :]
    for a in range(3):
        for h in range(2):
            toks[a, h, pl.ds(pl.multiple_of(place * half, half), half), :] = token_rows(a, pl.ds(h * half, half))[...]

    def group(w, d):
        if d == 0:
            for step in range(1, plane):
                src = level * plane + (place + step) % plane
                arrived(w, src)
                for way in (1, -1):
                    send_on(w, src, block(w, src), way)
            return
        for way in (1, -1):
            other = level - way * d

            @pl.when(jnp.logical_and(other >= 0, other < planes))
            def _():
                @pl.loop(0, plane)
                def _(q):
                    src = other * plane + q
                    arrived(w, src)
                    send_on(w, src, block(w, src), way)

    def relays(a):
        for step in range(1, plane):
            q = (place + step) % plane
            tok_arrived(a, q)
            relay(a, q).start()

    def relays_in(a):
        for step in range(1, plane):
            relayed(a, (place + step) % plane)

    def project(a, w, out):
        @pl.loop(0, 2)
        def _(h):
            out[h] = wide_dot(toks[a, h], weights[w])

    for d in range(planes - 1):
        for w in range(3):
            group(w, d)
    for a in range(3):
        relays(a)
    for a in range(3):
        relays_in(a)
    group(0, planes - 1)
    project(0, 0, back_gate)
    project(1, 0, fwd_gate)
    group(1, planes - 1)
    project(0, 1, back_up)
    project(1, 1, fwd_up)

    piece = 64

    @pl.loop(0, 2)
    def _(h):
        @pl.loop(0, slab // piece)
        def _(r):
            at = pl.ds(pl.multiple_of(r * piece, piece), piece)
            gate = fwd_gate[h, at, :]
            hidden[h, at, :] = (gate * jax.nn.sigmoid(gate) * fwd_up[h, at, :]).astype(jnp.bfloat16)
            gate = back_gate[h, at, :]
            s = jax.nn.sigmoid(gate)
            back_gate[h, at, :] = gate * s
            back_up[h, at, :] = back_up[h, at, :] * s * (1.0 + gate * (1.0 - s))

    group(2, planes - 1)

    @pl.loop(0, 2)
    def _(h):
        back = 0.5 * wide_dot(toks[2, h], weights[2])
        fwd_gate[h] = back
        gate_diff[pl.ds(pl.multiple_of(h * slab, slab), slab), :] = (back * back_up[h]).astype(jnp.bfloat16)
        up_diff[pl.ds(pl.multiple_of(h * slab, slab), slab), :] = (back * back_gate[h]).astype(jnp.bfloat16)

    def grad_hop(b, way):
        sends, recvs, lands = (lift_send, lift_recv, lifted) if way > 0 else (drop_send, drop_recv, dropped)
        to = (fs + way * plane + n_fs) % n_fs
        return remote(grad_send.at[b], lands.at[b], sends.at[b], recvs.at[b], (to, core))

    diff_turned = gate_diff[...].T

    for step in range(planes):
        there = jnp.where(2 * level < planes, planes - 1 - step, step)
        cols = pl.ds(pl.multiple_of(there * plane * depth, plane * depth), plane * depth)
        product = jnp.dot(diff_turned[:, :slab], toks[0, 0, :, cols], preferred_element_type=jnp.float32)
        product = product + jnp.dot(diff_turned[:, slab:], toks[0, 1, :, cols], preferred_element_type=jnp.float32)
        product = product.astype(jnp.bfloat16)
        for q in range(plane):
            grad_send[there * plane + q] = product[:, q * depth : (q + 1) * depth]
        for way, first in ((1, 0), (-1, planes - 1)):

            @pl.when(jnp.logical_and(level == first, there != first))
            def _():
                for q in range(plane):
                    grad_hop(there * plane + q, way).start()

    def serve(i):
        for way in (1, -1):
            lands = lifted if way > 0 else dropped
            there = planes - 1 - i if way > 0 else i
            left = (there - level) * way

            @pl.when(jnp.logical_and(can[-way], left >= 0))
            def _():
                @pl.loop(0, plane)
                def _(q):
                    b = there * plane + q
                    grad_hop(b, way).wait_recv()
                    total = grad_send[b].astype(jnp.float32) + lands[b].astype(jnp.float32)
                    grad_send[b] = total.astype(jnp.bfloat16)

                    @pl.when(left > 0)
                    def _():
                        grad_hop(b, way).start()

    def turn(step):
        q = (place + step) % plane
        return remote(grad_send.at[level * plane + q], grad_recv.at[place], turn_send.at[step], turn_recv.at[place], (level * plane + q, core))

    def cross(k):
        return remote(part.at[k, 1 - core], crossed.at[k], cross_sem.at[k, 0], cross_sem.at[k, 1], sibling)

    def join(k, step):
        q = (place + step) % plane
        return remote(joined.at[k, q], gathered.at[k, place], join_send.at[k, step], join_recv.at[k, place], (level * plane + q, core))

    strip = 512

    def partial(k, h):
        rows_at = pl.ds(pl.multiple_of(h * slab, slab), slab)

        @pl.loop(0, width // strip)
        def _(t):
            at = pl.ds(pl.multiple_of(t * strip, strip), strip)
            if k == 0:
                value = jnp.dot(hidden[h], weights[2, :, at], preferred_element_type=jnp.float32)
            else:
                value = jnp.dot(gate_diff[rows_at, :], weights[0, :, at], preferred_element_type=jnp.float32)
                value = value + jnp.dot(up_diff[rows_at, :], weights[1, :, at], preferred_element_type=jnp.float32)
            part[k, h, :, at] = value.astype(jnp.bfloat16)

    for k in range(2):
        partial(k, 1 - core)
        cross(k).start()
    for k in range(2):
        partial(k, core)
    for k in range(2):
        cross(k).wait_recv()
        for step in range(plane):
            q = (place + step + 1) % plane
            at = pl.ds(pl.multiple_of(q * half, half), half)
            total = part[k, core, at, :].astype(jnp.float32) + crossed[k, at, :].astype(jnp.float32)
            joined[k, q] = total.astype(jnp.bfloat16)
            if step < plane - 1:
                join(k, step + 1).start()
    for i in range(planes):
        serve(i)
    for step in range(1, plane):
        turn(step).start()
    grad_recv[place] = grad_send[fs]
    for k in range(2):
        gathered[k, place] = joined[k, place]

    mine = pl.ds(pl.multiple_of(core * half, half), half)

    def last(k):
        out = (fwd_out, back_out)[k]
        return remote(out.at[mine, :], out.at[mine, :], last_sem.at[k, 0], last_sem.at[k, 1], sibling)

    def joined_in(k):
        for step in range(1, plane):
            q = (place + step) % plane
            remote(joined.at[k, q], gathered.at[k, q], join_send.at[k, 0], join_recv.at[k, q], sibling).wait_recv()

    def total_of(k, at):
        value = gathered[k, 0, at, :].astype(jnp.float32)
        for q in range(1, plane):
            value = value + gathered[k, q, at, :].astype(jnp.float32)
        return value

    small = 16
    joined_in(0)
    for r in range(half // small):
        at = pl.ds(r * small, small)
        fwd_out[pl.ds(pl.multiple_of(core * half + r * small, small), small), :] = (0.5 * total_of(0, at)).astype(jnp.bfloat16)
    joined_in(1)
    for r in range(half // small):
        at = pl.ds(r * small, small)
        there = pl.ds(pl.multiple_of(core * half + r * small, small), small)
        values = tokens_ref[there, :].astype(jnp.float32)
        factor = lax.rsqrt(jnp.mean(values * values, axis=-1, keepdims=True) + norm_eps)
        scaled = total_of(1, at) * gain_ref[...]
        cubed = factor * factor * factor
        back_out[there, :] = (
            factor * scaled - values * cubed * jnp.mean(scaled * values, axis=-1, keepdims=True)
        ).astype(jnp.bfloat16)
    for k in range(2):
        last(k).start()

    for step in range(1, plane):
        q = (place + step) % plane
        remote(grad_send.at[fs], grad_recv.at[q], turn_send.at[0], turn_recv.at[q], sibling).wait_recv()
    for q in range(plane):
        grad_cols[q * rows : (q + 1) * rows, :] = grad_recv[q].astype(jnp.float32)

    @pl.loop(0, grad_cols.shape[0] // 128)
    def _(t):
        at = pl.ds(pl.multiple_of(t * 128, 128), 128)
        sum_out[:, at] = sum_ref[:, at] + grad_cols[at, :].T

    for w in range(3):
        for step in range(1, plane):
            staged(w, step).wait_send()
        for way in (1, -1):
            for d in range(planes - 1):
                other = level - way * d

                @pl.when(jnp.logical_and(can[way], jnp.logical_and(other >= 0, other < planes)))
                def _():
                    @pl.loop(0, plane)
                    def _(q):
                        src = other * plane + q
                        hop(w, src, block(w, src), way).wait_send()

    for a in range(3):
        for step in range(1, plane):
            tok_copy(a, step).wait_send()
            relay(a, (place + step) % plane).wait_send()
    for step in range(1, plane):
        turn(step).wait_send()
    for way in (1, -1):

        @pl.when(can[way])
        def _():
            @pl.loop(0, planes)
            def _(there):
                @pl.when((there - level) * way > 0)
                def _():
                    @pl.loop(0, plane)
                    def _(q):
                        grad_hop(there * plane + q, way).wait_send()

    for k in range(2):
        cross(k).wait_send()
        for step in range(1, plane):
            join(k, step).wait_send()
        last(k).wait()


def fused_shards(
    planes, plane, fwd_tokens, back_tokens, out_grad, norm_gain, gate_weight, up_weight, down_weight, gate_grad_sum
):
    tokens, width = fwd_tokens.shape
    depth, cols = gate_weight.shape
    rows = cols // plane
    half = tokens // 2
    slab = half * plane
    n_fs = planes * plane
    narrow, full = jnp.bfloat16, jnp.float32
    dma = pltpu.SemaphoreType.DMA
    vmem = pl.BlockSpec(memory_space=pltpu.VMEM)
    return pl.pallas_call(
        functools.partial(layer_kernel, planes, plane),
        out_shape=(
            jax.ShapeDtypeStruct((tokens, width), narrow),
            jax.ShapeDtypeStruct((tokens, width), narrow),
            jax.ShapeDtypeStruct((depth, cols), full),
        ),
        in_specs=[vmem] * 8,
        out_specs=(vmem,) * 3,
        scratch_shapes=[
            pltpu.VMEM((3, cols, depth), narrow),
            pltpu.VMEM((2, tokens, width), narrow),
            pltpu.VMEM((3, 2, slab, width), narrow),
            pltpu.VMEM((3, rows, width), narrow),
            pltpu.VMEM((2, slab, rows), full),
            pltpu.VMEM((2, slab, rows), full),
            pltpu.VMEM((2, slab, rows), full),
            pltpu.VMEM((2, slab, rows), full),
            pltpu.VMEM((2, slab, rows), narrow),
            pltpu.VMEM((2 * slab, rows), narrow),
            pltpu.VMEM((2 * slab, rows), narrow),
            pltpu.VMEM((2, 2, slab, width), narrow),
            pltpu.VMEM((2, slab, width), narrow),
            pltpu.VMEM((2, plane, half, width), narrow),
            pltpu.VMEM((2, plane, half, width), narrow),
            pltpu.VMEM((n_fs, rows, depth), narrow),
            pltpu.VMEM((n_fs, rows, depth), narrow),
            pltpu.VMEM((n_fs, rows, depth), narrow),
            pltpu.VMEM((plane, rows, depth), narrow),
            pltpu.VMEM((cols, depth), full),
            dma((3, plane)),
            dma((3, n_fs)),
            dma((3, n_fs)),
            dma((3, n_fs)),
            dma((3, plane)),
            dma((3, plane)),
            dma((3, plane)),
            dma((3, plane)),
            dma((n_fs,)),
            dma((n_fs,)),
            dma((n_fs,)),
            dma((n_fs,)),
            dma((plane,)),
            dma((plane,)),
            dma((2, 2)),
            dma((2, plane)),
            dma((2, plane)),
            dma((2, 2)),
        ],
        compiler_params=pltpu.CompilerParams(
            collective_id=0, has_side_effects=True, vmem_limit_bytes=56 * 2**20
        ),
    )(
        fwd_tokens, back_tokens, out_grad, norm_gain.reshape(1, width),
        gate_weight, up_weight, down_weight, gate_grad_sum,
    )


def square_side(count):
    side = 1
    while side * side * 4 <= count:
        side *= 2
    return side


def body_for(mesh):
    n_fs, plane = mesh.shape["fs"], square_side(mesh.shape["fs"])

    def body(*args):
        tokens, width = args[0].shape
        depth, cols = args[4].shape
        fits = (
            mesh.shape["tp"] == 2 and n_fs % plane == 0 and n_fs // plane >= 3 and plane >= 2
            and depth == 128 and cols % (plane * 16) == 0 and cols % 128 == 0
            and tokens % 128 == 0 and width % 512 == 0
        )
        if not fits:
            return shards(*args)
        return fused_shards(n_fs // plane, plane, *args)

    return body


def solution(mesh):
    in_specs = (
        P("fs", None),
        P("fs", None),
        P("fs", None),
        P(),
        P("fs", "tp"),
        P("fs", "tp"),
        P("fs", "tp"),
        P("fs", "tp"),
    )
    out_specs = (P("fs", None), P("fs", None), P("fs", "tp"))
    return jax.shard_map(body_for(mesh), mesh=mesh, in_specs=in_specs, out_specs=out_specs, check_vma=False)
```

```python
import functools

import jax
import jax.numpy as jnp
from jax import lax
from jax.experimental import pallas as pl
from jax.experimental.pallas import tpu as pltpu
from jax.sharding import PartitionSpec as P

norm_eps = 0.25


def normalize(tokens, norm_gain):
    values = tokens.astype(jnp.float32)
    factor = lax.rsqrt(jnp.mean(values * values, axis=-1, keepdims=True) + norm_eps)
    return (values, factor, (values * factor * norm_gain).astype(jnp.bfloat16))


def shards(
    fwd_tokens, back_tokens, out_grad, norm_gain, gate_weight, up_weight, down_weight, gate_grad_sum
):
    fwd_normed = normalize(fwd_tokens, norm_gain)[2]
    columns = fwd_normed
    gate_pre = jnp.dot(
        columns,
        lax.all_gather(gate_weight, "fs", axis=0, tiled=True),
        preferred_element_type=jnp.float32,
    )
    up_pre = jnp.dot(
        columns,
        lax.all_gather(up_weight, "fs", axis=0, tiled=True),
        preferred_element_type=jnp.float32,
    )
    hidden = (gate_pre * jax.nn.sigmoid(gate_pre) * up_pre).astype(jnp.bfloat16)
    partial_value = jnp.dot(
        hidden,
        lax.all_gather(down_weight, "fs", axis=0, tiled=True).T,
        preferred_element_type=jnp.float32,
    )
    summed = lax.psum(partial_value.astype(jnp.bfloat16), "tp").astype(jnp.float32)
    fwd_out = (0.5 * summed).astype(jnp.bfloat16)
    gate_whole = lax.all_gather(gate_weight, "fs", axis=0, tiled=True)
    up_whole = lax.all_gather(up_weight, "fs", axis=0, tiled=True)
    down_whole = lax.all_gather(down_weight, "fs", axis=0, tiled=True)
    values, factor, back_normed = normalize(back_tokens, norm_gain)
    gate_pre = jnp.dot(back_normed, gate_whole, preferred_element_type=jnp.float32)
    up_pre = jnp.dot(back_normed, up_whole, preferred_element_type=jnp.float32)
    sigmoid_gate = jax.nn.sigmoid(gate_pre)
    back_hidden = 0.5 * jnp.dot(out_grad, down_whole, preferred_element_type=jnp.float32)
    gate_diff = (
        back_hidden * up_pre * sigmoid_gate * (1.0 + gate_pre * (1.0 - sigmoid_gate))
    ).astype(jnp.bfloat16)
    up_diff = (back_hidden * gate_pre * sigmoid_gate).astype(jnp.bfloat16)
    columns = back_normed
    gate_grad_out = gate_grad_sum + lax.psum_scatter(
        jnp.dot(columns.T, gate_diff, preferred_element_type=jnp.float32),
        "fs",
        scatter_dimension=0,
        tiled=True,
    )
    partial_diff = jnp.dot(gate_diff, gate_whole.T, preferred_element_type=jnp.float32)
    partial_diff = partial_diff + jnp.dot(up_diff, up_whole.T, preferred_element_type=jnp.float32)
    normed_diff = lax.psum(partial_diff.astype(jnp.bfloat16), "tp").astype(jnp.float32)
    scaled = normed_diff * norm_gain
    cubed = factor * factor * factor
    back_grad = (
        factor * scaled - values * cubed * jnp.mean(scaled * values, axis=-1, keepdims=True)
    ).astype(jnp.bfloat16)
    back_grad, gate_grad_out = (back_grad, gate_grad_out)
    return (fwd_out, back_grad, gate_grad_out)


MESH = pl.DeviceIdType.MESH


def wide_dot(a, b):
    return lax.dot_general(a, b, (((1,), (1,)), ((), ())), preferred_element_type=jnp.float32)


def layer_kernel(
    planes, plane, fwd_ref, tokens_ref, grad_ref, gain_ref, gate_ref, up_ref, down_ref, sum_ref,
    fwd_out, back_out, sum_out,
    turned, normed, toks, weights, fwd_gate, fwd_up, back_gate, back_up, hidden, gate_diff, up_diff,
    part, crossed, joined, gathered, grad_send, lifted, dropped, grad_recv, grad_cols,
    stage_sem, weight_sem, up_sem, down_sem, tok_send, tok_recv, relay_send, relay_recv,
    lift_send, lift_recv, drop_send, drop_recv, turn_send, turn_recv, cross_sem, join_send, join_recv, last_sem,
):
    n_fs = planes * plane
    fs, core = lax.axis_index("fs"), lax.axis_index("tp")
    level, place = fs // plane, fs % plane
    sibling = (fs, 1 - core)
    rows = weights.shape[1]
    depth = gate_ref.shape[0]
    half = fwd_ref.shape[0] // 2
    slab = half * plane
    width = fwd_ref.shape[1]

    barrier = pltpu.get_barrier_semaphore()
    for step in range(1, plane):
        to = level * plane + (place + step) % plane
        pl.semaphore_signal(barrier, inc=1, device_id=(to, core), device_id_type=MESH)
    for step in (1, planes - 1):
        to = (fs + step * plane) % n_fs
        pl.semaphore_signal(barrier, inc=1, device_id=(to, core), device_id_type=MESH)
    pl.semaphore_signal(barrier, inc=1, device_id=sibling, device_id_type=MESH)

    @pl.loop(0, turned.shape[1] // 128)
    def _(t):
        at = pl.ds(pl.multiple_of(t * 128, 128), 128)
        turned[0, at, :] = gate_ref[:, at].T
        turned[1, at, :] = up_ref[:, at].T
        turned[2, at, :] = down_ref[:, at].T

    @pl.loop(0, fwd_ref.shape[0] // 16)
    def _(r):
        at = pl.ds(pl.multiple_of(r * 16, 16), 16)
        for a, ref in ((0, tokens_ref), (1, fwd_ref)):
            normed[a, at, :] = normalize(ref[at, :], gain_ref[...])[2]

    pl.semaphore_wait(barrier, plane + 2)

    def remote(src, dst, send, recv, device):
        return pltpu.make_async_remote_copy(
            src_ref=src, dst_ref=dst, send_sem=send, recv_sem=recv, device_id=device, device_id_type=MESH
        )

    def own_block(w, q):
        return turned.at[w, pl.ds(pl.multiple_of(q * rows, rows), rows), :]

    def block(w, src):
        return weights.at[w, :, pl.ds(pl.multiple_of(src * depth, depth), depth)]

    def staged(w, step):
        q = (place + step) % plane
        return remote(own_block(w, q), block(w, fs), stage_sem.at[w, step], weight_sem.at[w, fs], (level * plane + q, core))

    def arrived(w, src):
        remote(block(w, src), block(w, src), stage_sem.at[w, 0], weight_sem.at[w, src], sibling).wait_recv()

    def hop(w, src, source, step):
        sem = up_sem if step > 0 else down_sem
        return remote(source, block(w, src), sem.at[w, src], weight_sem.at[w, src], ((fs + step * plane + n_fs) % n_fs, core))

    can = {1: level < planes - 1, -1: level > 0}

    def send_on(w, src, source, step):
        @pl.when(can[step])
        def _():
            hop(w, src, source, step).start()

    def token_rows(a, at):
        return grad_ref.at[at, :] if a == 2 else normed.at[a, at, :]

    def tok_block(a, h, q):
        return toks.at[a, h, pl.ds(pl.multiple_of(q * half, half), half), :]

    def tok_copy(a, step):
        q = (place + step) % plane
        return remote(
            token_rows(a, pl.ds(pl.multiple_of(core * half, half), half)),
            tok_block(a, core, place), tok_send.at[a, step], tok_recv.at[a, place], (level * plane + q, core),
        )

    def tok_arrived(a, q):
        remote(tok_block(a, core, q), tok_block(a, core, q), tok_send.at[a, 0], tok_recv.at[a, q], sibling).wait_recv()

    def relay(a, q):
        return remote(tok_block(a, core, q), tok_block(a, core, q), relay_send.at[a, q], relay_recv.at[a, q], sibling)

    def relayed(a, q):
        remote(tok_block(a, 1 - core, q), tok_block(a, 1 - core, q), relay_send.at[a, q], relay_recv.at[a, q], sibling).wait_recv()

    for w in range(3):
        for step in range(1, plane):
            staged(w, step).start()
        for step in (1, -1):
            send_on(w, fs, own_block(w, place), step)
    for a in range(3):
        for step in range(1, plane):
            tok_copy(a, step).start()
    for w in range(3):
        weights[w, :, pl.ds(pl.multiple_of(fs * depth, depth), depth)] = turned[w, pl.ds(pl.multiple_of(place * rows, rows), rows), :]
    for a in range(3):
        for h in range(2):
            toks[a, h, pl.ds(pl.multiple_of(place * half, half), half), :] = token_rows(a, pl.ds(h * half, half))[...]

    def group(w, d):
        if d == 0:
            for step in range(1, plane):
                src = level * plane + (place + step) % plane
                arrived(w, src)
                for way in (1, -1):
                    send_on(w, src, block(w, src), way)
            return
        for way in (1, -1):
            other = level - way * d

            @pl.when(jnp.logical_and(other >= 0, other < planes))
            def _():
                @pl.loop(0, plane)
                def _(q):
                    src = other * plane + q
                    arrived(w, src)
                    send_on(w, src, block(w, src), way)

    def relays(a):
        for step in range(1, plane):
            q = (place + step) % plane
            tok_arrived(a, q)
            relay(a, q).start()

    def relays_in(a):
        for step in range(1, plane):
            relayed(a, (place + step) % plane)

    def project(a, w, out):
        @pl.loop(0, 2)
        def _(h):
            out[h] = wide_dot(toks[a, h], weights[w])

    for d in range(planes - 1):
        for w in range(3):
            group(w, d)
    for a in range(3):
        relays(a)
    for a in range(3):
        relays_in(a)
    group(0, planes - 1)
    project(0, 0, back_gate)
    project(1, 0, fwd_gate)
    group(1, planes - 1)
    project(0, 1, back_up)
    project(1, 1, fwd_up)

    piece = 64

    @pl.loop(0, 2)
    def _(h):
        @pl.loop(0, slab // piece)
        def _(r):
            at = pl.ds(pl.multiple_of(r * piece, piece), piece)
            gate = fwd_gate[h, at, :]
            hidden[h, at, :] = (gate * jax.nn.sigmoid(gate) * fwd_up[h, at, :]).astype(jnp.bfloat16)
            gate = back_gate[h, at, :]
            s = jax.nn.sigmoid(gate)
            back_gate[h, at, :] = gate * s
            back_up[h, at, :] = back_up[h, at, :] * s * (1.0 + gate * (1.0 - s))

    group(2, planes - 1)

    @pl.loop(0, 2)
    def _(h):
        back = 0.5 * wide_dot(toks[2, h], weights[2])
        fwd_gate[h] = back
        gate_diff[pl.ds(pl.multiple_of(h * slab, slab), slab), :] = (back * back_up[h]).astype(jnp.bfloat16)
        up_diff[pl.ds(pl.multiple_of(h * slab, slab), slab), :] = (back * back_gate[h]).astype(jnp.bfloat16)

    def grad_hop(b, way):
        sends, recvs, lands = (lift_send, lift_recv, lifted) if way > 0 else (drop_send, drop_recv, dropped)
        to = (fs + way * plane + n_fs) % n_fs
        return remote(grad_send.at[b], lands.at[b], sends.at[b], recvs.at[b], (to, core))

    diff_turned = gate_diff[...].T

    for step in range(planes):
        there = jnp.where(2 * level < planes, planes - 1 - step, step)
        cols = pl.ds(pl.multiple_of(there * plane * depth, plane * depth), plane * depth)
        product = jnp.dot(diff_turned[:, :slab], toks[0, 0, :, cols], preferred_element_type=jnp.float32)
        product = product + jnp.dot(diff_turned[:, slab:], toks[0, 1, :, cols], preferred_element_type=jnp.float32)
        product = product.astype(jnp.bfloat16)
        for q in range(plane):
            grad_send[there * plane + q] = product[:, q * depth : (q + 1) * depth]
        for way, first in ((1, 0), (-1, planes - 1)):

            @pl.when(jnp.logical_and(level == first, there != first))
            def _():
                for q in range(plane):
                    grad_hop(there * plane + q, way).start()

    def serve(i):
        for way in (1, -1):
            lands = lifted if way > 0 else dropped
            there = planes - 1 - i if way > 0 else i
            left = (there - level) * way

            @pl.when(jnp.logical_and(can[-way], left >= 0))
            def _():
                @pl.loop(0, plane)
                def _(q):
                    b = there * plane + q
                    grad_hop(b, way).wait_recv()
                    total = grad_send[b].astype(jnp.float32) + lands[b].astype(jnp.float32)
                    grad_send[b] = total.astype(jnp.bfloat16)

                    @pl.when(left > 0)
                    def _():
                        grad_hop(b, way).start()

    def turn(step):
        q = (place + step) % plane
        return remote(grad_send.at[level * plane + q], grad_recv.at[place], turn_send.at[step], turn_recv.at[place], (level * plane + q, core))

    def cross(k):
        return remote(part.at[k, 1 - core], crossed.at[k], cross_sem.at[k, 0], cross_sem.at[k, 1], sibling)

    def join(k, step):
        q = (place + step) % plane
        return remote(joined.at[k, q], gathered.at[k, place], join_send.at[k, step], join_recv.at[k, place], (level * plane + q, core))

    strip = 512

    def partial(k, h):
        rows_at = pl.ds(pl.multiple_of(h * slab, slab), slab)

        @pl.loop(0, width // strip)
        def _(t):
            at = pl.ds(pl.multiple_of(t * strip, strip), strip)
            if k == 0:
                value = jnp.dot(hidden[h], weights[2, :, at], preferred_element_type=jnp.float32)
            else:
                value = jnp.dot(gate_diff[rows_at, :], weights[0, :, at], preferred_element_type=jnp.float32)
                value = value + jnp.dot(up_diff[rows_at, :], weights[1, :, at], preferred_element_type=jnp.float32)
            part[k, h, :, at] = value.astype(jnp.bfloat16)

    for k in range(2):
        partial(k, 1 - core)
        cross(k).start()
    for k in range(2):
        partial(k, core)
    for k in range(2):
        cross(k).wait_recv()
        for step in range(plane):
            q = (place + step + 1) % plane
            at = pl.ds(pl.multiple_of(q * half, half), half)
            total = part[k, core, at, :].astype(jnp.float32) + crossed[k, at, :].astype(jnp.float32)
            joined[k, q] = total.astype(jnp.bfloat16)
            if step < plane - 1:
                join(k, step + 1).start()
    for i in range(planes):
        serve(i)
    for step in range(1, plane):
        turn(step).start()
    grad_recv[place] = grad_send[fs]
    for k in range(2):
        gathered[k, place] = joined[k, place]

    mine = pl.ds(pl.multiple_of(core * half, half), half)

    def last(k):
        out = (fwd_out, back_out)[k]
        return remote(out.at[mine, :], out.at[mine, :], last_sem.at[k, 0], last_sem.at[k, 1], sibling)

    def joined_in(k):
        for step in range(1, plane):
            q = (place + step) % plane
            remote(joined.at[k, q], gathered.at[k, q], join_send.at[k, 0], join_recv.at[k, q], sibling).wait_recv()

    def total_of(k, at):
        value = gathered[k, 0, at, :].astype(jnp.float32)
        for q in range(1, plane):
            value = value + gathered[k, q, at, :].astype(jnp.float32)
        return value

    small = 16
    joined_in(0)
    for r in range(half // small):
        at = pl.ds(r * small, small)
        fwd_out[pl.ds(pl.multiple_of(core * half + r * small, small), small), :] = (0.5 * total_of(0, at)).astype(jnp.bfloat16)
    joined_in(1)
    for r in range(half // small):
        at = pl.ds(r * small, small)
        there = pl.ds(pl.multiple_of(core * half + r * small, small), small)
        values = tokens_ref[there, :].astype(jnp.float32)
        factor = lax.rsqrt(jnp.mean(values * values, axis=-1, keepdims=True) + norm_eps)
        scaled = total_of(1, at) * gain_ref[...]
        cubed = factor * factor * factor
        back_out[there, :] = (
            factor * scaled - values * cubed * jnp.mean(scaled * values, axis=-1, keepdims=True)
        ).astype(jnp.bfloat16)
    for k in range(2):
        last(k).start()

    for step in range(1, plane):
        q = (place + step) % plane
        remote(grad_send.at[fs], grad_recv.at[q], turn_send.at[0], turn_recv.at[q], sibling).wait_recv()
    for q in range(plane):
        grad_cols[q * rows : (q + 1) * rows, :] = grad_recv[q].astype(jnp.float32)

    @pl.loop(0, grad_cols.shape[0] // 128)
    def _(t):
        at = pl.ds(pl.multiple_of(t * 128, 128), 128)
        sum_out[:, at] = sum_ref[:, at] + grad_cols[at, :].T

    for w in range(3):
        for step in range(1, plane):
            staged(w, step).wait_send()
        for way in (1, -1):
            for d in range(planes - 1):
                other = level - way * d

                @pl.when(jnp.logical_and(can[way], jnp.logical_and(other >= 0, other < planes)))
                def _():
                    @pl.loop(0, plane)
                    def _(q):
                        src = other * plane + q
                        hop(w, src, block(w, src), way).wait_send()

    for a in range(3):
        for step in range(1, plane):
            tok_copy(a, step).wait_send()
            relay(a, (place + step) % plane).wait_send()
    for step in range(1, plane):
        turn(step).wait_send()
    for way in (1, -1):

        @pl.when(can[way])
        def _():
            @pl.loop(0, planes)
            def _(there):
                @pl.when((there - level) * way > 0)
                def _():
                    @pl.loop(0, plane)
                    def _(q):
                        grad_hop(there * plane + q, way).wait_send()

    for k in range(2):
        cross(k).wait_send()
        for step in range(1, plane):
            join(k, step).wait_send()
        last(k).wait()


def fused_shards(
    planes, plane, fwd_tokens, back_tokens, out_grad, norm_gain, gate_weight, up_weight, down_weight, gate_grad_sum
):
    tokens, width = fwd_tokens.shape
    depth, cols = gate_weight.shape
    rows = cols // plane
    half = tokens // 2
    slab = half * plane
    n_fs = planes * plane
    narrow, full = jnp.bfloat16, jnp.float32
    dma = pltpu.SemaphoreType.DMA
    vmem = pl.BlockSpec(memory_space=pltpu.VMEM)
    return pl.pallas_call(
        functools.partial(layer_kernel, planes, plane),
        out_shape=(
            jax.ShapeDtypeStruct((tokens, width), narrow),
            jax.ShapeDtypeStruct((tokens, width), narrow),
            jax.ShapeDtypeStruct((depth, cols), full),
        ),
        in_specs=[vmem] * 8,
        out_specs=(vmem,) * 3,
        scratch_shapes=[
            pltpu.VMEM((3, cols, depth), narrow),
            pltpu.VMEM((2, tokens, width), narrow),
            pltpu.VMEM((3, 2, slab, width), narrow),
            pltpu.VMEM((3, rows, width), narrow),
            pltpu.VMEM((2, slab, rows), full),
            pltpu.VMEM((2, slab, rows), full),
            pltpu.VMEM((2, slab, rows), full),
            pltpu.VMEM((2, slab, rows), full),
            pltpu.VMEM((2, slab, rows), narrow),
            pltpu.VMEM((2 * slab, rows), narrow),
            pltpu.VMEM((2 * slab, rows), narrow),
            pltpu.VMEM((2, 2, slab, width), narrow),
            pltpu.VMEM((2, slab, width), narrow),
            pltpu.VMEM((2, plane, half, width), narrow),
            pltpu.VMEM((2, plane, half, width), narrow),
            pltpu.VMEM((n_fs, rows, depth), narrow),
            pltpu.VMEM((n_fs, rows, depth), narrow),
            pltpu.VMEM((n_fs, rows, depth), narrow),
            pltpu.VMEM((plane, rows, depth), narrow),
            pltpu.VMEM((cols, depth), full),
            dma((3, plane)),
            dma((3, n_fs)),
            dma((3, n_fs)),
            dma((3, n_fs)),
            dma((3, plane)),
            dma((3, plane)),
            dma((3, plane)),
            dma((3, plane)),
            dma((n_fs,)),
            dma((n_fs,)),
            dma((n_fs,)),
            dma((n_fs,)),
            dma((plane,)),
            dma((plane,)),
            dma((2, 2)),
            dma((2, plane)),
            dma((2, plane)),
            dma((2, 2)),
        ],
        compiler_params=pltpu.CompilerParams(
            collective_id=0, has_side_effects=True, vmem_limit_bytes=56 * 2**20
        ),
    )(
        fwd_tokens, back_tokens, out_grad, norm_gain.reshape(1, width),
        gate_weight, up_weight, down_weight, gate_grad_sum,
    )


def square_side(count):
    side = 1
    while side * side * 4 <= count:
        side *= 2
    return side


def body_for(mesh):
    n_fs, plane = mesh.shape["fs"], square_side(mesh.shape["fs"])

    def body(*args):
        tokens, width = args[0].shape
        depth, cols = args[4].shape
        fits = (
            mesh.shape["tp"] == 2 and n_fs % plane == 0 and n_fs // plane >= 3 and plane >= 2
            and depth == 128 and cols % (plane * 16) == 0 and cols % 128 == 0
            and tokens % 128 == 0 and width % 512 == 0
        )
        if not fits:
            return shards(*args)
        return fused_shards(n_fs // plane, plane, *args)

    return body


def solution(mesh):
    in_specs = (
        P("fs", None),
        P("fs", None),
        P("fs", None),
        P(),
        P("fs", "tp"),
        P("fs", "tp"),
        P("fs", "tp"),
        P("fs", "tp"),
    )
    out_specs = (P("fs", None), P("fs", None), P("fs", "tp"))
    return jax.shard_map(body_for(mesh), mesh=mesh, in_specs=in_specs, out_specs=out_specs, check_vma=False)
```
